32 devices in a mesh: sp: 8 (over z, x), tp: 4 (over y, core).
Axes of the slice: x: 2, y: 2, z: 4, core: 2. Of those that a mesh axis runs over, the one named last changes fastest.
Arguments:
- q_first: bfloat16 [1536, 512], P('sp', 'tp'), may hold values from -6 to 6
- k_first: bfloat16 [1536, 512], P('sp', 'tp'), may hold values from -6 to 6
- q_second: bfloat16 [1536, 512], P('sp', 'tp'), may hold values from -6 to 6
- k_second: bfloat16 [1536, 512], P('sp', 'tp'), may hold values from -6 to 6
- values: bfloat16 [1536, 1024], P('sp', 'tp'), may hold values from -6 to 6
- lambdas: float32 [8], P('tp'), may hold values from 0.3 to 0.8
- head_gain: float32 [128], replicated, may hold values from 0.1 to 1.9
- out_weight: bfloat16 [1024, 2048], P('tp'), may hold values from -0.1875 to 0.1875
- residual_in: bfloat16 [1536, 2048], P('sp'), may hold values from -6 to 6
- mix_gain: float32 [2048], replicated, may hold values from 0.1 to 1.9
- gate_weight: bfloat16 [2048, 5632], P('sp', 'tp'), may hold values from -0.125 to 0.125
- up_weight: bfloat16 [2048, 5632], P('sp', 'tp'), may hold values from -0.125 to 0.125
- gate_taps: float32 [3, 5632], P(None, 'tp'), may hold values from -3.5 to 3.5
- up_taps: float32 [3, 5632], P(None, 'tp'), may hold values from -3.5 to 3.5
- down_weight: bfloat16 [5632, 2048], P('tp'), may hold values from -0.078125 to 0.078125
Outputs:
- mixed: bfloat16 [1536, 2048], P(('sp', 'tp'))
The draws below stay inside these ranges and needn't reach their ends.
All inputs are finite; a program needn't handle non-finite values.
Results may differ from the reference program's by a relative error of at most 0.017.
Values may be sent and summed in bfloat16 or wider, within the bound.
No kernel may reach another device: no remote copies, remote signals or barrier semaphores. Data moves between devices by JAX's collectives and lax.ppermute only.
A program may use at most 128 MiB of HBM per device.

```python
import math
import jax
import jax.numpy as jnp
from jax import lax

D = 2048
HEADS = 8
HEAD_DIM = 64
VALUE_DIM = 128
FF = 5632
KERNEL = 3
TOKENS = 1536


def aligned_pair(key):
    shape = (TOKENS, HEADS * HEAD_DIM)
    query_key = jax.random.fold_in(key, 71)
    other_key = jax.random.fold_in(key, 72)
    queries = jnp.clip(1.35 * jax.random.normal(query_key, shape, jnp.float32), -6.0, 6.0)
    keys = jnp.clip(1.35 * jax.random.normal(other_key, shape, jnp.float32), -6.0, 6.0)
    return (queries.astype(jnp.bfloat16), keys.astype(jnp.bfloat16))


def draw_q_first(key, part):
    return aligned_pair(key)[0]


def draw_k_first(key, part):
    return aligned_pair(key)[1]


def shard_levels(own_key, extent, pieces, low, top_value):
    loudness = 1.0
    for position, shards_of in pieces:
        heights = jax.random.uniform(jax.random.fold_in(jax.random.fold_in(own_key, 6), position), (shards_of,), jnp.float32, low / len(pieces), top_value / len(pieces))
        loudness = loudness * jnp.repeat(jnp.exp(heights), extent[position] // shards_of).reshape((-1,) + (1,) * (len(extent) - 1 - position))
    return loudness


def normal_values(key, dims, spread, limit, split=(), kind=jnp.bfloat16):
    entries = spread * jax.random.normal(key, dims, jnp.float32)
    if split:
        entries = entries * shard_levels(key, dims, split, -0.22, 0.18)
    return jnp.clip(entries, -limit, limit).astype(kind)


def setup_inputs(seed: int = 0) -> dict:
    arg_keys = jax.random.split(jax.random.key(seed), 16)
    return {
        "q_first": draw_q_first(jax.random.fold_in(arg_keys[15], 71), 0),
        "k_first": draw_k_first(jax.random.fold_in(arg_keys[15], 71), 0),
        "q_second": normal_values(arg_keys[2], (TOKENS, HEADS * HEAD_DIM), 1.35, 6.0, ((0, 8), (1, 4))),
        "k_second": normal_values(arg_keys[3], (TOKENS, HEADS * HEAD_DIM), 1.35, 6.0, ((0, 8), (1, 4))),
        "values": normal_values(arg_keys[4], (TOKENS, HEADS * VALUE_DIM), 1.0, 6.0, ((0, 8), (1, 4))),
        "lambdas": jnp.clip(0.3 + 0.5 * jax.random.uniform(arg_keys[5], (HEADS,), jnp.float32) ** shard_levels(arg_keys[5], (HEADS,), ((0, 4),), -0.2, 0.2), 0.3, 0.8),
        "head_gain": jnp.clip(1.0 + 0.18 * jax.random.normal(arg_keys[6], (VALUE_DIM,), jnp.float32), 0.1, 1.9),
        "out_weight": normal_values(arg_keys[7], (HEADS * VALUE_DIM, D), (HEADS * VALUE_DIM) ** -0.5, 0.1875, ((0, 4),)),
        "residual_in": normal_values(arg_keys[8], (TOKENS, D), 1.0, 6.0, ((0, 8),)),
        "mix_gain": jnp.clip(1.0 + 0.18 * jax.random.normal(arg_keys[9], (D,), jnp.float32), 0.1, 1.9),
        "gate_weight": normal_values(arg_keys[10], (D, FF), D ** -0.5, 0.125, ((0, 8), (1, 4))),
        "up_weight": normal_values(arg_keys[11], (D, FF), D ** -0.5, 0.125, ((0, 8), (1, 4))),
        "gate_taps": normal_values(arg_keys[12], (KERNEL, FF), KERNEL ** -0.5, 3.5, ((1, 4),), jnp.float32),
        "up_taps": normal_values(arg_keys[13], (KERNEL, FF), KERNEL ** -0.5, 3.5, ((1, 4),), jnp.float32),
        "down_weight": normal_values(arg_keys[14], (FF, D), FF ** -0.5, 0.078125, ((0, 4),)),
    }


norm_eps = 1e-06
far_below = -1e+30

def reference(q_first, k_first, q_second, k_second, values, lambdas, head_gain, out_weight, residual_in, mix_gain, gate_weight, up_weight, gate_taps, up_taps, down_weight):
    total = q_first.shape[0]
    scale = HEAD_DIM ** (-0.5)
    query_a = q_first.astype(jnp.float32).reshape(total, HEADS, HEAD_DIM)
    query_b = q_second.astype(jnp.float32).reshape(total, HEADS, HEAD_DIM)
    keys_a = k_first.astype(jnp.float32).reshape(total, HEADS, HEAD_DIM)
    keys_b = k_second.astype(jnp.float32).reshape(total, HEADS, HEAD_DIM)
    vals = values.astype(jnp.float32).reshape(total, HEADS, VALUE_DIM)
    block_rows = math.gcd(total, 512)
    key_pos = jnp.arange(total, dtype=jnp.int32)

    def weigh(queries, keys, visible):
        scores = jnp.einsum('qhd,khd->hqk', queries, keys, precision=lax.Precision.HIGHEST) * scale
        masked = jnp.where(visible, scores, far_below)
        peak = lax.optimization_barrier(jnp.max(masked, axis=-1, keepdims=True))
        expo = jnp.where(visible, jnp.exp(masked - peak), 0.0)
        totals = lax.optimization_barrier(jnp.sum(expo, axis=-1))
        rounded = expo.astype(jnp.bfloat16).astype(jnp.float32)
        accum = jnp.einsum('hqk,khv->qhv', rounded, vals, precision=lax.Precision.HIGHEST)
        return accum / totals.T[..., None]

    def attend(block_index):
        row_start = (block_index * block_rows).astype(jnp.int32)
        query_pos = row_start + jnp.arange(block_rows, dtype=jnp.int32)
        visible = (key_pos[None, :] <= query_pos[:, None])[None]
        first = weigh(lax.dynamic_slice_in_dim(query_a, row_start, block_rows, 0), keys_a, visible)
        second = weigh(lax.dynamic_slice_in_dim(query_b, row_start, block_rows, 0), keys_b, visible)
        diff_heads = first - lambdas[None, :, None] * second
        normed = diff_heads * lax.rsqrt(lax.optimization_barrier(jnp.mean(diff_heads * diff_heads, axis=-1, keepdims=True)) + norm_eps) * head_gain
        return normed.astype(jnp.bfloat16).reshape(block_rows, HEADS * VALUE_DIM)
    head_out = lax.map(attend, jnp.arange(total // block_rows, dtype=jnp.int32)).reshape(total, HEADS * VALUE_DIM)
    attended = jnp.dot(head_out, out_weight, preferred_element_type=jnp.float32)
    stream = residual_in.astype(jnp.float32) + attended
    ffn_in = (stream * lax.rsqrt(lax.optimization_barrier(jnp.mean(stream * stream, axis=-1, keepdims=True)) + norm_eps) * mix_gain).astype(jnp.bfloat16)
    gate_pre = jnp.dot(ffn_in, gate_weight, preferred_element_type=jnp.float32).astype(jnp.bfloat16)
    up_pre = jnp.dot(ffn_in, up_weight, preferred_element_type=jnp.float32).astype(jnp.bfloat16)

    def convolve(projected, taps):
        padded = jnp.pad(projected.astype(jnp.float32), ((KERNEL - 1, 0), (0, 0)))
        result = taps[0][None, :] * padded[0:total]
        for offset in range(1, KERNEL):
            result = result + taps[offset][None, :] * padded[offset:offset + total]
        return result
    gate_conv = convolve(gate_pre, gate_taps)
    up_conv = convolve(up_pre, up_taps)
    hidden = (jax.nn.silu(gate_conv) * up_conv).astype(jnp.bfloat16)
    return (stream + jnp.dot(hidden, down_weight, preferred_element_type=jnp.float32)).astype(jnp.bfloat16)
```

```python
import jax
import jax.numpy as jnp
from jax import lax
from jax.sharding import PartitionSpec as P


norm_eps = 1e-06
far_below = -1e30
HALO_TILE = 16


def snake(count):
    return list(range(0, count, 2)) + list(range(count - 1 - count % 2, 0, -2))


def ring_gather(value, axis):
    count = lax.axis_size(axis)
    order = snake(count)
    rank = lax.axis_index(axis)
    table = jnp.array(order, jnp.int32)
    place = jnp.array([order.index(i) for i in range(count)], jnp.int32)[rank]
    down = [(order[i], order[(i + 1) % count]) for i in range(count)]
    up = [(target, source) for source, target in down]
    blocks = [(value, rank)]
    from_low = from_high = value
    for step in range(1, (count - 1) // 2 + 1):
        from_low = lax.ppermute(from_low, axis, down)
        from_high = lax.ppermute(from_high, axis, up)
        blocks.append((from_low, table[(place - step) % count]))
        blocks.append((from_high, table[(place + step) % count]))
    if count % 2 == 0:
        half = value.shape[0] // 2
        first = lax.ppermute(from_low[:half], axis, down)
        second = lax.ppermute(from_high[half:], axis, up)
        far = jnp.concatenate((first, second), axis=0)
        blocks.append((far, table[(place + count // 2) % count]))
    return blocks


def swapped(value, axis, bit):
    count = lax.axis_size(axis)
    return lax.ppermute(value, axis, [(i, i ^ bit) for i in range(count)])


def xor_gather(value, axis):
    count = lax.axis_size(axis)
    blocks = [value]
    slots = {0: value}
    bits = [1 << b for b in range((count - 1).bit_length())]
    for bit in reversed(bits):
        slots.update({slot | bit: swapped(block, axis, bit) for slot, block in list(slots.items())})
    return [slots[i] for i in range(count)]


def rms_scale(field, gain):
    return field * lax.rsqrt(jnp.mean(field * field, axis=-1, keepdims=True) + norm_eps) * gain


def weigh(queries, keys, vals, visible, scale):
    scores = jnp.einsum("qhd,khd->hqk", queries, keys, preferred_element_type=jnp.float32) * scale
    masked = jnp.where(visible, scores, far_below)
    peaks = jnp.max(masked, axis=-1, keepdims=True)
    weights = jnp.where(visible, jnp.exp(masked - peaks), 0.0)
    totals = jnp.sum(weights, axis=-1)
    accum = jnp.einsum(
        "hqk,khv->qhv", weights.astype(jnp.bfloat16), vals, preferred_element_type=jnp.float32
    )
    return accum / totals.T[..., None]


def shards(
    q_first,
    k_first,
    q_second,
    k_second,
    values,
    lambdas,
    head_gain,
    out_weight,
    residual_in,
    mix_gain,
    gate_weight,
    up_weight,
    gate_taps,
    up_taps,
    down_weight,
):
    sp_count, tp_count = lax.axis_size("sp"), lax.axis_size("tp")
    sp_rank, tp_rank = lax.axis_index("sp"), lax.axis_index("tp")
    tok_rows = q_first.shape[0]
    head_count = lambdas.shape[0]
    key_width = q_first.shape[1]
    head_dim = key_width // head_count
    value_dim = values.shape[1] // head_count
    part_rows = tok_rows // tp_count
    tap_count = gate_taps.shape[0]
    halo = min(tok_rows, -(-(tap_count - 1) // HALO_TILE) * HALO_TILE)
    rows = tok_rows + halo
    width = gate_weight.shape[1]
    depth = gate_weight.shape[0]
    scale = head_dim ** (-0.5)

    own_kv = jnp.concatenate((k_first, k_second, values), axis=1)
    kv_blocks = ring_gather(own_kv, "sp")
    tail = jnp.concatenate((q_first, q_second, residual_in), axis=1)[tok_rows - halo :]
    before = lax.ppermute(tail, "sp", [(i, i + 1) for i in range(sp_count - 1)])
    out_rows = jnp.concatenate(xor_gather(out_weight, "tp"), axis=0)
    w_blocks = ring_gather(jnp.concatenate((gate_weight, up_weight), axis=1), "sp")

    query_pos = sp_rank * tok_rows - halo + jnp.arange(rows, dtype=jnp.int32)
    query_a = jnp.concatenate((before[:, :key_width], q_first), axis=0)
    query_b = jnp.concatenate((before[:, key_width : 2 * key_width], q_second), axis=0)
    residual = jnp.concatenate((before[:, 2 * key_width :], residual_in), axis=0)
    all_kv = jnp.concatenate([block for block, _ in kv_blocks], axis=0)
    offsets = jnp.arange(tok_rows, dtype=jnp.int32)
    key_pos = jnp.concatenate([source * tok_rows + offsets for _, source in kv_blocks])
    total = all_kv.shape[0]
    visible = (key_pos[None, :] <= jnp.maximum(query_pos, 0)[:, None])[None]
    vals = all_kv[:, 2 * key_width :].reshape(total, head_count, value_dim)
    first = weigh(
        query_a.reshape(rows, head_count, head_dim),
        all_kv[:, :key_width].reshape(total, head_count, head_dim),
        vals,
        visible,
        scale,
    )
    second = weigh(
        query_b.reshape(rows, head_count, head_dim),
        all_kv[:, key_width : 2 * key_width].reshape(total, head_count, head_dim),
        vals,
        visible,
        scale,
    )
    diff_heads = first - lambdas[None, :, None] * second
    head_out = (
        rms_scale(diff_heads, head_gain)
        .astype(jnp.bfloat16)
        .reshape(rows, head_count * value_dim)
    )
    heads = jnp.concatenate(xor_gather(head_out, "tp"), axis=1)
    attended = jnp.dot(heads, out_rows, preferred_element_type=jnp.float32)
    stream = residual.astype(jnp.float32) + attended
    ffn_in = rms_scale(stream, mix_gain).astype(jnp.bfloat16)

    projected = None
    for block, source in w_blocks:
        columns = lax.dynamic_slice_in_dim(ffn_in, source * depth, depth, 1)
        product = jnp.dot(columns, block, preferred_element_type=jnp.float32)
        projected = product if projected is None else projected + product
    projected = jnp.where(query_pos[:, None] >= 0, projected.astype(jnp.bfloat16), 0.0)
    projected = projected.astype(jnp.float32)
    taps = jnp.concatenate((gate_taps, up_taps), axis=1)
    lead = halo - (tap_count - 1)
    convolved = taps[0][None] * projected[lead : lead + tok_rows]
    for offset in range(1, tap_count):
        start = lead + offset
        convolved = convolved + taps[offset][None] * projected[start : start + tok_rows]
    hidden = (jax.nn.silu(convolved[:, :width]) * convolved[:, width:]).astype(jnp.bfloat16)
    partial = jnp.dot(hidden, down_weight, preferred_element_type=jnp.float32).astype(jnp.bfloat16)

    def part_of(array, start, part):
        return lax.dynamic_slice_in_dim(array, start + part * part_rows, part_rows, 0)

    mixed = part_of(stream, halo, tp_rank) + part_of(partial, 0, tp_rank).astype(jnp.float32)
    for bit in range(tp_count - 1, 0, -1):
        mixed = mixed + swapped(part_of(partial, 0, tp_rank ^ bit), "tp", bit).astype(jnp.float32)
    return mixed.astype(jnp.bfloat16)


def solution(mesh):
    in_specs = (
        P("sp", "tp"),
        P("sp", "tp"),
        P("sp", "tp"),
        P("sp", "tp"),
        P("sp", "tp"),
        P("tp"),
        P(),
        P("tp", None),
        P("sp", None),
        P(),
        P("sp", "tp"),
        P("sp", "tp"),
        P(None, "tp"),
        P(None, "tp"),
        P("tp", None),
    )
    out_specs = P(("sp", "tp"), None)
    return jax.shard_map(shards, mesh=mesh, in_specs=in_specs, out_specs=out_specs, check_vma=False)
```

```python
import functools

import jax
import jax.numpy as jnp
from jax import lax
from jax.experimental import pallas as pl
from jax.experimental.pallas import tpu as pltpu
from jax.sharding import PartitionSpec as P


norm_eps = 1e-06
far_below = -1e30
HALO_TILE = 16


def swapped(value, axis, bit):
    count = lax.axis_size(axis)
    return lax.ppermute(value, axis, [(i, i ^ bit) for i in range(count)])


def xor_gather(value, axis):
    count = lax.axis_size(axis)
    blocks = [value]
    slots = {0: value}
    bits = [1 << b for b in range((count - 1).bit_length())]
    for bit in reversed(bits):
        slots.update({slot | bit: swapped(block, axis, bit) for slot, block in list(slots.items())})
    return [slots[i] for i in range(count)]


def rms_scale(field, gain):
    return field * lax.rsqrt(jnp.mean(field * field, axis=-1, keepdims=True) + norm_eps) * gain


def whole(count):
    return [pl.BlockSpec(memory_space=pltpu.VMEM)] * count


def params_for(mebibytes):
    return pltpu.CompilerParams(vmem_limit_bytes=mebibytes * 2**20)


def attend_kernel(head_count, block_count, scale, *refs):
    where_ref, lambda_ref, before_ref, qa_ref, qb_ref = refs[:5]
    kv_refs = refs[5 : 5 + block_count]
    gain_ref, out_ref, key_ref, query_ref, score_ref = refs[5 + block_count :]
    tok_rows, key_width = qa_ref.shape
    rows = out_ref.shape[0]
    halo = rows - tok_rows
    head_dim = key_width // head_count
    value_dim = out_ref.shape[1] // head_count
    for b, kv_ref in enumerate(kv_refs):
        key_ref[b * tok_rows : (b + 1) * tok_rows, :] = kv_ref[...]
    for m, ref in enumerate((qa_ref, qb_ref)):
        columns = slice(m * key_width, (m + 1) * key_width)
        query_ref[:halo, columns] = before_ref[:, columns]
        query_ref[halo:, columns] = ref[...]
    shape = (rows, tok_rows)
    ahead = lax.broadcasted_iota(jnp.int32, shape, 0) - halo
    spread = jnp.maximum(ahead + where_ref[0] * tok_rows, 0) - lax.broadcasted_iota(
        jnp.int32, shape, 1
    )
    for h in range(head_count):
        results = []
        for m in range(2):
            start = m * key_width + h * head_dim
            query = query_ref[:, start : start + head_dim]
            peak = None
            for b in range(block_count):
                span = slice(b * tok_rows, (b + 1) * tok_rows)
                scores = lax.dot_general(
                    query,
                    key_ref[span, start : start + head_dim],
                    (((1,), (1,)), ((), ())),
                    preferred_element_type=jnp.float32,
                )
                source = where_ref[b]
                limit = jnp.where(source >= 0, source * tok_rows, 2**30)
                scores = jnp.where(spread >= limit, scores * scale, far_below)
                score_ref[b] = scores
                top = jnp.max(scores, axis=-1, keepdims=True)
                peak = top if peak is None else jnp.maximum(peak, top)
            total = accum = None
            for b in range(block_count):
                span = slice(b * tok_rows, (b + 1) * tok_rows)
                first = 2 * key_width + h * value_dim
                weights = jnp.exp(score_ref[b] - peak)
                amount = jnp.sum(weights, axis=-1, keepdims=True)
                product = jnp.dot(
                    weights.astype(jnp.bfloat16),
                    key_ref[span, first : first + value_dim],
                    preferred_element_type=jnp.float32,
                )
                total = amount if b == 0 else total + amount
                accum = product if b == 0 else accum + product
            results.append(accum / total)
        field = results[0] - lambda_ref[h] * results[1]
        norm = lax.rsqrt(jnp.mean(field * field, axis=-1, keepdims=True) + norm_eps)
        out_ref[:, h * value_dim : (h + 1) * value_dim] = (field * norm * gain_ref[...]).astype(
            out_ref.dtype
        )


def attend(where, lambdas, before, q_first, q_second, blocks, head_gain, head_count, width):
    tok_rows, key_width = q_first.shape
    rows = tok_rows + before.shape[0]
    count = len(blocks)
    scale = (key_width // head_count) ** (-0.5)
    keys = count * tok_rows
    smem = pl.BlockSpec(memory_space=pltpu.SMEM)
    return pl.pallas_call(
        functools.partial(attend_kernel, head_count, count, scale),
        out_shape=jax.ShapeDtypeStruct((rows, width), jnp.bfloat16),
        in_specs=[smem, smem] + whole(4 + count),
        out_specs=pl.BlockSpec(memory_space=pltpu.VMEM),
        scratch_shapes=[
            pltpu.VMEM((keys, blocks[0].shape[1]), jnp.bfloat16),
            pltpu.VMEM((rows, 2 * key_width), jnp.bfloat16),
            pltpu.VMEM((count, rows, tok_rows), jnp.float32),
        ],
        compiler_params=params_for(48),
        cost_estimate=pl.CostEstimate(
            flops=4 * rows * keys * (key_width + width),
            bytes_accessed=2 * keys * blocks[0].shape[1],
            transcendentals=2 * head_count * rows * keys,
        ),
        name="attend",
    )(where, lambdas, before, q_first, q_second, *blocks, head_gain[None])


def project_kernel(slots, part_rows, where_ref, *refs):
    head_refs, weight_refs = refs[:slots], refs[slots : 2 * slots]
    before_ref, residual_ref, gain_ref, part_ref, first_ref, rest_ref, stream_ref = refs[2 * slots :]
    halo = before_ref.shape[0]
    total = None
    for head_ref, weight_ref in zip(head_refs, weight_refs):
        product = jnp.dot(head_ref[...], weight_ref[...], preferred_element_type=jnp.float32)
        total = product if total is None else total + product
    stream_ref[:halo] = total[:halo] + before_ref[...].astype(jnp.float32)
    stream_ref[halo:] = total[halo:] + residual_ref[...].astype(jnp.float32)
    rank = where_ref[0]
    part_ref[...] = stream_ref[pl.ds(pl.multiple_of(halo + rank * part_rows, 8), part_rows), :]
    stream = stream_ref[...]
    norm = lax.rsqrt(jnp.mean(stream * stream, axis=-1, keepdims=True) + norm_eps)
    quarter = first_ref.shape[1]
    for slot in range(slots):
        columns = pl.ds(pl.multiple_of((rank ^ slot) * quarter, 128), quarter)
        piece = (stream_ref[:, columns] * norm * gain_ref[:, columns]).astype(jnp.bfloat16)
        if slot == 0:
            first_ref[...] = piece
        else:
            rest_ref[slot - 1] = piece


def project(rank, heads, weights, before, residual, gain):
    slots = len(heads)
    rows = heads[0].shape[0]
    tok_rows, columns = residual.shape
    part = tok_rows // slots
    quarter = columns // slots
    vmem = pl.BlockSpec(memory_space=pltpu.VMEM)
    return pl.pallas_call(
        functools.partial(project_kernel, slots, part),
        out_shape=(
            jax.ShapeDtypeStruct((part, columns), jnp.float32),
            jax.ShapeDtypeStruct((rows, quarter), jnp.bfloat16),
            jax.ShapeDtypeStruct((slots - 1, rows, quarter), jnp.bfloat16),
        ),
        in_specs=[pl.BlockSpec(memory_space=pltpu.SMEM)] + whole(2 * slots + 3),
        out_specs=(vmem,) * 3,
        scratch_shapes=[pltpu.VMEM((rows, columns), jnp.float32)],
        compiler_params=params_for(48),
        cost_estimate=pl.CostEstimate(
            flops=2 * rows * columns * slots * heads[0].shape[1],
            bytes_accessed=2 * columns * slots * heads[0].shape[1],
            transcendentals=rows,
        ),
        name="project",
    )(rank, *heads, *weights, before, residual, gain[None])


def mixer_kernel(slots, sides, taken, tok_rows, where_ref, *refs):
    piece_refs = refs[:taken]
    weight_ref, taps_ref, out_ref, pre_ref = refs[taken:]
    tap_count = taps_ref.shape[0]
    rows = pre_ref.shape[0]
    share = out_ref.shape[1]
    halo = rows - tok_rows
    layer, side, rank, source = (where_ref[i] for i in range(4))
    layers = weight_ref.shape[0] // sides
    depth = weight_ref.shape[1]
    pieces = []
    for ref in piece_refs:
        pieces += [ref] if len(ref.shape) == 2 else [ref.at[i] for i in range(ref.shape[0])]
    total = None
    per_slot = pieces[0].shape[1] // depth
    for slot, piece in enumerate(pieces):
        for i in range(per_slot):
            row_block = (rank ^ slot) * per_slot + i
            index = lax.rem(layer + layers - row_block // sides, layers) * sides
            index = index + (side ^ (row_block % sides))
            product = jnp.dot(
                piece[:, i * depth : (i + 1) * depth],
                weight_ref[index],
                preferred_element_type=jnp.float32,
            )
            total = product if total is None else total + product
    position = lax.broadcasted_iota(jnp.int32, (rows, 1), 0) - halo + source * tok_rows
    total = jnp.where(position >= 0, total, 0.0)
    pre_ref[...] = total.astype(jnp.bfloat16).astype(jnp.float32)
    lead = halo - (tap_count - 1)
    convolved = None
    for k in range(tap_count):
        term = taps_ref[k : k + 1, :] * pre_ref[lead + k : lead + k + tok_rows, :]
        convolved = term if convolved is None else convolved + term
    gate = convolved[:, :share]
    out_ref[...] = (gate / (1.0 + jnp.exp(-gate)) * convolved[:, share:]).astype(out_ref.dtype)


def mixer(where, pieces, weight, taps, slots, sides, tok_rows):
    rows = pieces[0].shape[-2]
    columns = weight.shape[2]
    return pl.pallas_call(
        functools.partial(mixer_kernel, slots, sides, len(pieces), tok_rows),
        out_shape=jax.ShapeDtypeStruct((tok_rows, columns // 2), jnp.bfloat16),
        in_specs=[pl.BlockSpec(memory_space=pltpu.SMEM)] + whole(len(pieces) + 2),
        out_specs=pl.BlockSpec(memory_space=pltpu.VMEM),
        scratch_shapes=[pltpu.VMEM((rows, columns), jnp.float32)],
        compiler_params=params_for(32),
        cost_estimate=pl.CostEstimate(
            flops=2 * rows * columns * weight.shape[0] * weight.shape[1],
            bytes_accessed=2 * columns * weight.shape[0] * weight.shape[1],
            transcendentals=rows * columns // 2,
        ),
        name="mixer",
    )(where, *pieces, weight, taps)


def layers_of(sp_count, tp_count):
    if sp_count > 8 or sp_count % 2 or tp_count & (tp_count - 1):
        return None
    layers = sp_count // 2
    if layers < 2 or (2 * layers) % tp_count:
        return None
    return layers, 2


def halo_of(tok_rows, tap_count):
    return min(tok_rows, -(-(tap_count - 1) // HALO_TILE) * HALO_TILE)


def weigh(queries, keys, vals, visible, scale):
    scores = jnp.einsum("qhd,khd->hqk", queries, keys, preferred_element_type=jnp.float32) * scale
    masked = jnp.where(visible, scores, far_below)
    peaks = jnp.max(masked, axis=-1, keepdims=True)
    weights = jnp.where(visible, jnp.exp(masked - peaks), 0.0)
    totals = jnp.sum(weights, axis=-1)
    accum = jnp.einsum(
        "hqk,khv->qhv", weights.astype(jnp.bfloat16), vals, preferred_element_type=jnp.float32
    )
    return accum / totals.T[..., None]


def local_shards(
    q_first,
    k_first,
    q_second,
    k_second,
    values,
    lambdas,
    head_gain,
    out_weight,
    residual_in,
    mix_gain,
    gate_weight,
    up_weight,
    gate_taps,
    up_taps,
    down_weight,
):
    sp_count, tp_count = lax.axis_size("sp"), lax.axis_size("tp")
    sp_rank, tp_rank = lax.axis_index("sp"), lax.axis_index("tp")
    tok_rows = q_first.shape[0]
    head_count = lambdas.shape[0]
    key_width = q_first.shape[1]
    head_dim = key_width // head_count
    value_dim = values.shape[1] // head_count
    tap_count, width = gate_taps.shape
    halo = halo_of(tok_rows, tap_count)
    rows = tok_rows + halo
    scale = head_dim ** (-0.5)
    own_kv = jnp.concatenate((k_first, k_second, values), axis=1)
    all_kv = lax.all_gather(own_kv, "sp", axis=0, tiled=True)
    tail = jnp.concatenate((q_first, q_second, residual_in), axis=1)[tok_rows - halo :]
    before = lax.ppermute(tail, "sp", [(i, i + 1) for i in range(sp_count - 1)])
    out_rows = lax.all_gather(out_weight, "tp", axis=0, tiled=True)
    gates = lax.all_gather(gate_weight, "sp", axis=0, tiled=True)
    ups = lax.all_gather(up_weight, "sp", axis=0, tiled=True)
    query_pos = sp_rank * tok_rows - halo + jnp.arange(rows, dtype=jnp.int32)
    query_a = jnp.concatenate((before[:, :key_width], q_first), axis=0)
    query_b = jnp.concatenate((before[:, key_width : 2 * key_width], q_second), axis=0)
    residual = jnp.concatenate((before[:, 2 * key_width :], residual_in), axis=0)
    total = all_kv.shape[0]
    key_pos = jnp.arange(total, dtype=jnp.int32)
    visible = (key_pos[None, :] <= jnp.maximum(query_pos, 0)[:, None])[None]
    vals = all_kv[:, 2 * key_width :].reshape(total, head_count, value_dim)
    maps = [
        weigh(
            query.reshape(rows, head_count, head_dim),
            all_kv[:, m * key_width : (m + 1) * key_width].reshape(total, head_count, head_dim),
            vals,
            visible,
            scale,
        )
        for m, query in enumerate((query_a, query_b))
    ]
    diff_heads = maps[0] - lambdas[None, :, None] * maps[1]
    head_out = rms_scale(diff_heads, head_gain).astype(jnp.bfloat16)
    head_out = head_out.reshape(rows, head_count * value_dim)
    heads = lax.all_gather(head_out, "tp", axis=1, tiled=True)
    attended = jnp.dot(heads, out_rows, preferred_element_type=jnp.float32)
    stream = residual.astype(jnp.float32) + attended
    ffn_in = rms_scale(stream, mix_gain).astype(jnp.bfloat16)

    def convolve(weight, taps):
        projected = jnp.dot(ffn_in, weight, preferred_element_type=jnp.float32)
        projected = jnp.where(query_pos[:, None] >= 0, projected.astype(jnp.bfloat16), 0.0)
        projected = projected.astype(jnp.float32)
        lead = halo - (tap_count - 1)
        result = taps[0][None] * projected[lead : lead + tok_rows]
        for offset in range(1, tap_count):
            start = lead + offset
            result = result + taps[offset][None] * projected[start : start + tok_rows]
        return result

    hidden = jax.nn.silu(convolve(gates, gate_taps)) * convolve(ups, up_taps)
    down = jnp.dot(hidden.astype(jnp.bfloat16), down_weight, preferred_element_type=jnp.float32)
    summed = lax.psum_scatter(
        down.astype(jnp.bfloat16), "tp", scatter_dimension=0, tiled=True
    ).astype(jnp.float32)
    part_rows = tok_rows // tp_count
    own = lax.dynamic_slice_in_dim(stream, halo + tp_rank * part_rows, part_rows, 0)
    return (own + summed).astype(jnp.bfloat16)


def shards(
    q_first,
    k_first,
    q_second,
    k_second,
    values,
    lambdas,
    head_gain,
    out_weight,
    residual_in,
    mix_gain,
    gate_weight,
    up_weight,
    gate_taps,
    up_taps,
    down_weight,
):
    sp_count, tp_count = lax.axis_size("sp"), lax.axis_size("tp")
    sp_rank, tp_rank = lax.axis_index("sp"), lax.axis_index("tp")
    tok_rows = q_first.shape[0]
    head_count = lambdas.shape[0]
    key_width = q_first.shape[1]
    part_rows = tok_rows // tp_count
    tap_count = gate_taps.shape[0]
    halo = halo_of(tok_rows, tap_count)
    depth, width = gate_weight.shape
    layers, sides = layers_of(sp_count, tp_count)
    layer, side = sp_rank // sides, sp_rank % sides
    share = width // layers

    def across(value, up, flip, wrap=True, keep=lambda l, s: True):
        pairs = []
        for source in range(sp_count):
            l, s = source // sides, source % sides
            target = (l + up) % layers * sides + (s ^ flip)
            if keep(l, s) and (wrap or 0 <= l + up < layers):
                pairs.append((source, target))
        return lax.ppermute(value, "sp", pairs)

    own_kv = jnp.concatenate((k_first, k_second, values), axis=1)
    shifted = [own_kv] + [across(own_kv, k, 0, wrap=False) for k in range(1, layers)]
    blocks = [(own_kv, sp_rank)]
    for k, block in enumerate(shifted):
        if k > 0:
            blocks.append((block, sp_rank - k * sides))
        if sides == 2:
            useful = (lambda l, s: s == 0) if k == 0 else (lambda l, s, k=k: l >= k)
            other = (layer - k) * sides + (side ^ 1)
            blocks.append((across(block, 0, 1, keep=useful), other))
    gate, hold = lax.optimization_barrier((gate_weight, shifted[min(1, layers - 1)]))
    del hold
    tail = jnp.concatenate((q_first, q_second, residual_in), axis=1)[tok_rows - halo :]
    before = lax.ppermute(tail, "sp", [(i, i + 1) for i in range(sp_count - 1)])
    out_rows = xor_gather(out_weight, "tp")

    taps = jnp.concatenate((gate_taps, up_taps), axis=1)
    cuts = jnp.stack(
        [
            jnp.concatenate(
                (
                    gate[:, l * share : (l + 1) * share],
                    up_weight[:, l * share : (l + 1) * share],
                ),
                axis=1,
            )
            for l in range(layers)
        ]
    )
    slots = []
    for k in range(layers):
        cut = lax.dynamic_index_in_dim(cuts, (layer + k) % layers, 0, keepdims=False)
        block = across(cut, k, 0) if k else cut
        slots += [block, across(block, 0, 1)]
    weight = jnp.stack(slots)
    taps = lax.dynamic_slice_in_dim(
        taps.reshape(tap_count, 2, layers, share), layer, 1, 2
    ).reshape(tap_count, 2 * share)

    heads = attend(
        jnp.stack([source for _, source in blocks]),
        lambdas,
        before[:, : 2 * key_width],
        q_first,
        q_second,
        [block for block, _ in blocks],
        head_gain,
        head_count,
        values.shape[1],
    )
    own_stream, first_piece, other_pieces = project(
        tp_rank[None],
        xor_gather(heads, "tp"),
        out_rows,
        before[:, 2 * key_width :],
        residual_in,
        mix_gain,
    )
    arrived = [None] + [across(first_piece, k, 0) for k in range(1, layers)]
    down = None
    for k in range(layers):
        source = (layer - k) % layers * sides + side
        where = jnp.stack([layer, side, tp_rank, source])
        pieces = xor_gather(arrived[k], "tp") if k else [first_piece, other_pieces]
        hidden = mixer(where, pieces, weight, taps, tp_count, sides, tok_rows)
        if k:
            hidden = across(hidden, -k, 0)
        held = lax.dynamic_slice_in_dim(
            down_weight, (layer + k) % layers * share, share, 0
        )
        product = jnp.dot(hidden, held, preferred_element_type=jnp.float32)
        down = product if down is None else down + product
    partial = down.astype(jnp.bfloat16)

    def part_of(array, part):
        return lax.dynamic_slice_in_dim(array, part * part_rows, part_rows, 0)

    mixed = own_stream + part_of(partial, tp_rank).astype(jnp.float32)
    for bit in range(tp_count - 1, 0, -1):
        mixed = mixed + swapped(part_of(partial, tp_rank ^ bit), "tp", bit).astype(jnp.float32)
    return mixed.astype(jnp.bfloat16)


def solution(mesh):
    in_specs = (
        P("sp", "tp"),
        P("sp", "tp"),
        P("sp", "tp"),
        P("sp", "tp"),
        P("sp", "tp"),
        P("tp"),
        P(),
        P("tp", None),
        P("sp", None),
        P(),
        P("sp", "tp"),
        P("sp", "tp"),
        P(None, "tp"),
        P(None, "tp"),
        P("tp", None),
    )
    out_specs = P(("sp", "tp"), None)
    sizes = mesh.shape
    spread = layers_of(sizes["sp"], sizes["tp"])
    body = shards if spread else local_shards
    return jax.shard_map(body, mesh=mesh, in_specs=in_specs, out_specs=out_specs, check_vma=False)
```

```python
import functools

import jax
import jax.numpy as jnp
from jax import lax
from jax.experimental import pallas as pl
from jax.experimental.pallas import tpu as pltpu
from jax.sharding import PartitionSpec as P


norm_eps = 1e-06
far_below = -1e30
HALO_TILE = 16


def swapped(value, axis, bit):
    count = lax.axis_size(axis)
    return lax.ppermute(value, axis, [(i, i ^ bit) for i in range(count)])


def xor_gather(value, axis):
    count = lax.axis_size(axis)
    slots = {0: value}
    bits = [1 << b for b in range((count - 1).bit_length())]
    for bit in reversed(bits):
        for slot, block in list(slots.items()):
            slots[slot | bit] = swapped(block, axis, bit)
    return [slots[i] for i in range(count)]


def after(value, *others):
    return lax.optimization_barrier((value,) + others)[0]


def rms_scale(field, gain):
    return field * lax.rsqrt(jnp.mean(field * field, axis=-1, keepdims=True) + norm_eps) * gain


def whole(count):
    return [pl.BlockSpec(memory_space=pltpu.VMEM)] * count


def params_for(mebibytes):
    return pltpu.CompilerParams(vmem_limit_bytes=mebibytes * 2**20)


def attend_kernel(head_count, block_count, sides, scale, *refs):
    lambda_ref, before_ref, qa_ref, qb_ref = refs[:4]
    kv_refs = refs[4 : 4 + block_count]
    gain_ref, out_ref, key_ref, query_ref, score_ref, sems = refs[4 + block_count :]
    place = lax.axis_index("sp")
    layer, side = place // sides, lax.rem(place, sides)
    tok_rows, key_width = qa_ref.shape
    rows = out_ref.shape[0]
    halo = rows - tok_rows
    head_dim = key_width // head_count
    value_dim = out_ref.shape[1] // head_count
    copies = [
        pltpu.make_async_copy(
            ref, query_ref.at[pl.ds(halo, tok_rows), m * key_width : (m + 1) * key_width], sems.at[m]
        )
        for m, ref in enumerate((qa_ref, qb_ref))
    ]
    for copy in copies:
        copy.start()
    for b, kv_ref in enumerate(kv_refs):
        key_ref[b * tok_rows : (b + 1) * tok_rows, :] = kv_ref[...]
    query_ref[:halo, :] = before_ref[:, : 2 * key_width]
    for copy in copies:
        copy.wait()
    shape = (rows, tok_rows)
    ahead = lax.broadcasted_iota(jnp.int32, shape, 0) - halo
    spread = jnp.maximum(ahead + place * tok_rows, 0) - lax.broadcasted_iota(
        jnp.int32, shape, 1
    )
    for h in range(head_count):
        results = []
        for m in range(2):
            start = m * key_width + h * head_dim
            query = query_ref[:, start : start + head_dim]
            peak = None
            for b in range(block_count):
                span = slice(b * tok_rows, (b + 1) * tok_rows)
                scores = lax.dot_general(
                    query,
                    key_ref[span, start : start + head_dim],
                    (((1,), (1,)), ((), ())),
                    preferred_element_type=jnp.float32,
                )
                source = (layer - b // sides) * sides + (side ^ (b % sides))
                limit = jnp.where(source >= 0, source * tok_rows, 2**30)
                scores = jnp.where(spread >= limit, scores * scale, far_below)
                score_ref[b] = scores
                top = jnp.max(scores, axis=-1, keepdims=True)
                peak = top if peak is None else jnp.maximum(peak, top)
            total = accum = None
            for b in range(block_count):
                span = slice(b * tok_rows, (b + 1) * tok_rows)
                first = 2 * key_width + h * value_dim
                weights = jnp.exp(score_ref[b] - peak)
                amount = jnp.sum(weights, axis=-1, keepdims=True)
                product = jnp.dot(
                    weights.astype(jnp.bfloat16),
                    key_ref[span, first : first + value_dim],
                    preferred_element_type=jnp.float32,
                )
                total = amount if b == 0 else total + amount
                accum = product if b == 0 else accum + product
            results.append(accum / total)
        field = results[0] - lambda_ref[h] * results[1]
        norm = lax.rsqrt(jnp.mean(field * field, axis=-1, keepdims=True) + norm_eps)
        out_ref[:, h * value_dim : (h + 1) * value_dim] = (field * norm * gain_ref[...]).astype(
            out_ref.dtype
        )


def attend(lambdas, before, q_first, q_second, blocks, head_gain, head_count, width, sides):
    tok_rows, key_width = q_first.shape
    rows = tok_rows + before.shape[0]
    count = len(blocks)
    scale = (key_width // head_count) ** (-0.5)
    keys = count * tok_rows
    smem = pl.BlockSpec(memory_space=pltpu.SMEM)
    return pl.pallas_call(
        functools.partial(attend_kernel, head_count, count, sides, scale),
        out_shape=jax.ShapeDtypeStruct((rows, width), jnp.bfloat16),
        in_specs=[smem]
        + whole(1)
        + [pl.BlockSpec(memory_space=pl.ANY)] * 2
        + whole(count + 1),
        out_specs=pl.BlockSpec(memory_space=pltpu.VMEM),
        scratch_shapes=[
            pltpu.VMEM((keys, blocks[0].shape[1]), jnp.bfloat16),
            pltpu.VMEM((rows, 2 * key_width), jnp.bfloat16),
            pltpu.VMEM((count, rows, tok_rows), jnp.float32),
            pltpu.SemaphoreType.DMA((2,)),
        ],
        compiler_params=params_for(60),
        cost_estimate=pl.CostEstimate(
            flops=4 * rows * keys * (key_width + width),
            bytes_accessed=2 * keys * blocks[0].shape[1],
            transcendentals=2 * head_count * rows * keys,
        ),
        name="attend",
    )(lambdas, before, q_first, q_second, *blocks, head_gain[None])


def project_kernel(slots, part_rows, *refs):
    head_refs, weight_refs = refs[:slots], refs[slots : 2 * slots]
    before_ref, residual_ref, gain_ref, part_ref, first_ref, rest_ref = refs[2 * slots :][:6]
    stream_ref, held_ref, own_ref, sems = refs[2 * slots + 6 :]
    own_copy = pltpu.make_async_copy(weight_refs[0], own_ref, sems.at[0])
    copy = pltpu.make_async_copy(residual_ref, held_ref, sems.at[1])
    own_copy.start()
    copy.start()
    halo, skip = before_ref.shape
    skip = skip - stream_ref.shape[1]
    total = None
    for slot in reversed(range(slots)):
        weight_ref = weight_refs[slot]
        if slot == 0:
            own_copy.wait()
            weight_ref = own_ref
        product = jnp.dot(
            head_refs[slot][...], weight_ref[...], preferred_element_type=jnp.float32
        )
        total = product if total is None else total + product
    stream_ref[:halo] = total[:halo] + before_ref[:, skip:].astype(jnp.float32)
    copy.wait()
    stream_ref[halo:] = total[halo:] + held_ref[...].astype(jnp.float32)
    rank = lax.axis_index("tp")
    part_ref[...] = stream_ref[pl.ds(pl.multiple_of(halo + rank * part_rows, 8), part_rows), :]
    stream = stream_ref[...]
    norm = lax.rsqrt(jnp.mean(stream * stream, axis=-1, keepdims=True) + norm_eps)
    quarter = first_ref.shape[1]
    for slot in range(slots):
        columns = pl.ds(pl.multiple_of((rank ^ slot) * quarter, 128), quarter)
        piece = (stream_ref[:, columns] * norm * gain_ref[:, columns]).astype(jnp.bfloat16)
        if slot == 0:
            first_ref[...] = piece
        else:
            rest_ref[slot - 1] = piece


def project(heads, weights, before, residual, gain):
    slots = len(heads)
    rows = heads[0].shape[0]
    tok_rows, columns = residual.shape
    part = tok_rows // slots
    quarter = columns // slots
    vmem = pl.BlockSpec(memory_space=pltpu.VMEM)
    return pl.pallas_call(
        functools.partial(project_kernel, slots, part),
        out_shape=(
            jax.ShapeDtypeStruct((part, columns), jnp.float32),
            jax.ShapeDtypeStruct((rows, quarter), jnp.bfloat16),
            jax.ShapeDtypeStruct((slots - 1, rows, quarter), jnp.bfloat16),
        ),
        in_specs=whole(2 * slots + 1)
        + [pl.BlockSpec(memory_space=pl.ANY), vmem],
        out_specs=(vmem,) * 3,
        scratch_shapes=[
            pltpu.VMEM((rows, columns), jnp.float32),
            pltpu.VMEM(residual.shape, residual.dtype),
            pltpu.VMEM(weights[0].shape, weights[0].dtype),
            pltpu.SemaphoreType.DMA((2,)),
        ],
        compiler_params=params_for(60),
        cost_estimate=pl.CostEstimate(
            flops=2 * rows * columns * slots * heads[0].shape[1],
            bytes_accessed=2 * columns * slots * heads[0].shape[1],
            transcendentals=rows,
        ),
        name="project",
    )(*heads, *weights, before, residual, gain[None])


def copy_all(pairs, sems):
    copies = [
        pltpu.make_async_copy(source, target, sems.at[i]) for i, (source, target) in enumerate(pairs)
    ]
    for copy in copies:
        copy.start()
    for copy in copies:
        copy.wait()


def pack_kernel(k_first_ref, k_second_ref, values_ref, qa_ref, qb_ref, rest_ref, kv_ref, tail_ref, sems):
    rows, width = k_first_ref.shape
    halo = tail_ref.shape[0]
    last = pl.ds(rows - halo, halo)
    copy_all(
        [
            (k_first_ref, kv_ref.at[:, :width]),
            (k_second_ref, kv_ref.at[:, width : 2 * width]),
            (values_ref, kv_ref.at[:, 2 * width :]),
            (qa_ref.at[last, :], tail_ref.at[:, :width]),
            (qb_ref.at[last, :], tail_ref.at[:, width : 2 * width]),
            (rest_ref.at[last, :], tail_ref.at[:, 2 * width :]),
        ],
        sems,
    )


def pack(k_first, k_second, values, q_first, q_second, residual, halo):
    tok_rows, width = k_first.shape
    return pl.pallas_call(
        pack_kernel,
        out_shape=(
            jax.ShapeDtypeStruct((tok_rows, 2 * width + values.shape[1]), k_first.dtype),
            jax.ShapeDtypeStruct((halo, 2 * width + residual.shape[1]), residual.dtype),
        ),
        in_specs=[pl.BlockSpec(memory_space=pl.ANY)] * 6,
        out_specs=tuple(whole(2)),
        scratch_shapes=[pltpu.SemaphoreType.DMA((6,))],
        compiler_params=params_for(60),
        name="pack",
    )(k_first, k_second, values, q_first, q_second, residual)


def cut_kernel(layers, sides, gate_ref, up_ref, gate_taps_ref, up_taps_ref, *refs):
    out_refs, (taps_ref, gate_held, up_held, sems) = refs[:layers], refs[layers:]
    share = gate_ref.shape[1] // layers
    copy_all([(gate_ref, gate_held), (up_ref, up_held)], sems)
    layer = lax.axis_index("sp") // sides
    for own in range(layers):

        @pl.when(layer == own)
        def _():
            for k, out_ref in enumerate(out_refs):
                start = (own + k) % layers * share
                out_ref[:, :share] = gate_held[:, start : start + share]
                out_ref[:, share:] = up_held[:, start : start + share]
            start = own * share
            taps_ref[:, :share] = gate_taps_ref[:, start : start + share]
            taps_ref[:, share:] = up_taps_ref[:, start : start + share]


def cut(gate_weight, up_weight, gate_taps, up_taps, layers, sides):
    depth, width = gate_weight.shape
    share = 2 * (width // layers)
    return pl.pallas_call(
        functools.partial(cut_kernel, layers, sides),
        out_shape=[jax.ShapeDtypeStruct((depth, share), gate_weight.dtype)] * layers
        + [jax.ShapeDtypeStruct((gate_taps.shape[0], share), gate_taps.dtype)],
        in_specs=[pl.BlockSpec(memory_space=pl.ANY)] * 2 + whole(2),
        out_specs=whole(layers + 1),
        scratch_shapes=[
            pltpu.VMEM(gate_weight.shape, gate_weight.dtype),
            pltpu.VMEM(up_weight.shape, up_weight.dtype),
            pltpu.SemaphoreType.DMA((2,)),
        ],
        compiler_params=params_for(60),
        cost_estimate=pl.CostEstimate(
            flops=4 * depth * width, bytes_accessed=8 * depth * width, transcendentals=0
        ),
        name="cut",
    )(gate_weight, up_weight, gate_taps, up_taps)


def mixer_kernel(slots, layers, sides, tok_rows, aboves, counts, *refs):
    count = layers * sides
    taken = sum(counts)
    piece_refs, weight_refs = refs[:taken], refs[taken : taken + count]
    taps_ref, *out_refs = refs[taken + count : -2]
    act_ref, pre_ref = refs[-2:]
    tap_count = taps_ref.shape[0]
    rows = pre_ref.shape[0]
    share = out_refs[0].shape[1]
    halo = rows - tok_rows
    place, rank = lax.axis_index("sp"), lax.axis_index("tp")
    layer, side = place // sides, lax.rem(place, sides)
    depth = weight_refs[0].shape[0]
    per_slot = count // slots
    begin = 0
    for above, number, out_ref in zip(aboves, counts, out_refs):
        pieces = []
        for ref in piece_refs[begin : begin + number]:
            pieces += [ref] if len(ref.shape) == 2 else [ref.at[i] for i in range(ref.shape[0])]
        begin += number
        for slot, piece in enumerate(pieces):
            for i in range(per_slot):
                act_ref[slot * per_slot + i] = piece[:, i * depth : (i + 1) * depth]
        total = None
        for j, weight_ref in enumerate(weight_refs):
            block = lax.rem(layer + layers - j // sides, layers) * sides + (side ^ (j % sides))
            slot = (block // per_slot) ^ rank
            act = act_ref[slot * per_slot + lax.rem(block, per_slot)]
            product = jnp.dot(act, weight_ref[...], preferred_element_type=jnp.float32)
            total = product if total is None else total + product
        source = lax.rem(layer + layers - above, layers) * sides + side
        position = lax.broadcasted_iota(jnp.int32, (rows, 1), 0) - halo + source * tok_rows
        total = jnp.where(position >= 0, total, 0.0)
        pre_ref[...] = total.astype(jnp.bfloat16).astype(jnp.float32)
        lead = halo - (tap_count - 1)
        convolved = None
        for k in range(tap_count):
            term = taps_ref[k : k + 1, :] * pre_ref[lead + k : lead + k + tok_rows, :]
            convolved = term if convolved is None else convolved + term
        gate = convolved[:, :share]
        out_ref[...] = (gate / (1.0 + jnp.exp(-gate)) * convolved[:, share:]).astype(out_ref.dtype)


def mixer(blocks, weights, taps, slots, layers, tok_rows):
    aboves = tuple(blocks)
    counts = tuple(len(pieces) for pieces in blocks.values())
    arrays = [piece for pieces in blocks.values() for piece in pieces]
    rows = arrays[0].shape[-2]
    depth, columns = weights[0].shape
    count = len(weights)
    return pl.pallas_call(
        functools.partial(
            mixer_kernel, slots, layers, count // layers, tok_rows, aboves, counts
        ),
        out_shape=[jax.ShapeDtypeStruct((tok_rows, columns // 2), jnp.bfloat16)] * len(aboves),
        in_specs=whole(len(arrays) + count + 1),
        out_specs=whole(len(aboves)),
        scratch_shapes=[
            pltpu.VMEM((count, rows, depth), jnp.bfloat16),
            pltpu.VMEM((rows, columns), jnp.float32),
        ],
        compiler_params=params_for(32),
        cost_estimate=pl.CostEstimate(
            flops=2 * len(aboves) * rows * columns * count * depth,
            bytes_accessed=2 * columns * count * depth,
            transcendentals=len(aboves) * rows * columns // 2,
        ),
        name="mixer",
    )(*arrays, *weights, taps)


def down_kernel(layers, sides, *refs):
    hidden_refs, (weight_ref, stream_ref), out_refs = refs[:layers], refs[layers : layers + 2], refs[layers + 2 :]
    own_ref, *part_refs = out_refs[:-1]
    total_ref = out_refs[-1]
    share = hidden_refs[0].shape[1]
    layer, rank = lax.axis_index("sp") // sides, lax.axis_index("tp")
    total = None
    for k, hidden_ref in enumerate(hidden_refs):
        start = pl.multiple_of(lax.rem(layer + k, layers) * share, 16)
        product = jnp.dot(
            hidden_ref[...], weight_ref[pl.ds(start, share), :], preferred_element_type=jnp.float32
        )
        total = product if total is None else total + product
    total_ref[...] = total
    rows = own_ref.shape[0]
    own_ref[...] = stream_ref[...] + total_ref[pl.ds(pl.multiple_of(rank * rows, 8), rows), :]
    for bit, part_ref in enumerate(part_refs, 1):
        start = pl.multiple_of((rank ^ bit) * rows, 8)
        part_ref[...] = total_ref[pl.ds(start, rows), :].astype(part_ref.dtype)


def project_down(hiddens, weight, stream, slots, sides):
    rows, columns = stream.shape
    layers = len(hiddens)
    return pl.pallas_call(
        functools.partial(down_kernel, layers, sides),
        out_shape=[jax.ShapeDtypeStruct(stream.shape, jnp.float32)]
        + [jax.ShapeDtypeStruct(stream.shape, jnp.bfloat16)] * (slots - 1),
        in_specs=whole(layers + 2),
        out_specs=whole(slots),
        scratch_shapes=[
            pltpu.VMEM((rows * slots, columns), jnp.float32),
        ],
        compiler_params=params_for(24),
        cost_estimate=pl.CostEstimate(
            flops=2 * rows * slots * weight.size,
            bytes_accessed=2 * weight.size,
            transcendentals=0,
        ),
        name="down",
    )(*hiddens, weight, stream)


def layers_of(sp_count, tp_count):
    if sp_count > 8 or sp_count % 2 or tp_count & (tp_count - 1):
        return None
    layers = sp_count // 2
    if layers < 2 or (2 * layers) % tp_count:
        return None
    return layers, 2


def halo_of(tok_rows, tap_count):
    return min(tok_rows, -(-(tap_count - 1) // HALO_TILE) * HALO_TILE)


def weigh(queries, keys, vals, visible, scale):
    scores = jnp.einsum("qhd,khd->hqk", queries, keys, preferred_element_type=jnp.float32) * scale
    masked = jnp.where(visible, scores, far_below)
    peaks = jnp.max(masked, axis=-1, keepdims=True)
    weights = jnp.where(visible, jnp.exp(masked - peaks), 0.0)
    totals = jnp.sum(weights, axis=-1)
    accum = jnp.einsum(
        "hqk,khv->qhv", weights.astype(jnp.bfloat16), vals, preferred_element_type=jnp.float32
    )
    return accum / totals.T[..., None]


def local_shards(
    q_first,
    k_first,
    q_second,
    k_second,
    values,
    lambdas,
    head_gain,
    out_weight,
    residual_in,
    mix_gain,
    gate_weight,
    up_weight,
    gate_taps,
    up_taps,
    down_weight,
):
    sp_count, tp_count = lax.axis_size("sp"), lax.axis_size("tp")
    sp_rank, tp_rank = lax.axis_index("sp"), lax.axis_index("tp")
    tok_rows = q_first.shape[0]
    head_count = lambdas.shape[0]
    key_width = q_first.shape[1]
    head_dim = key_width // head_count
    value_dim = values.shape[1] // head_count
    tap_count, _ = gate_taps.shape
    halo = halo_of(tok_rows, tap_count)
    rows = tok_rows + halo
    scale = head_dim ** (-0.5)
    own_kv = jnp.concatenate((k_first, k_second, values), axis=1)
    all_kv = lax.all_gather(own_kv, "sp", axis=0, tiled=True)
    tail = jnp.concatenate((q_first, q_second, residual_in), axis=1)[tok_rows - halo :]
    before = lax.ppermute(tail, "sp", [(i, i + 1) for i in range(sp_count - 1)])
    out_rows = lax.all_gather(out_weight, "tp", axis=0, tiled=True)
    gates = lax.all_gather(gate_weight, "sp", axis=0, tiled=True)
    ups = lax.all_gather(up_weight, "sp", axis=0, tiled=True)
    query_pos = sp_rank * tok_rows - halo + jnp.arange(rows, dtype=jnp.int32)
    query_a = jnp.concatenate((before[:, :key_width], q_first), axis=0)
    query_b = jnp.concatenate((before[:, key_width : 2 * key_width], q_second), axis=0)
    residual = jnp.concatenate((before[:, 2 * key_width :], residual_in), axis=0)
    total = all_kv.shape[0]
    key_pos = jnp.arange(total, dtype=jnp.int32)
    visible = (key_pos[None, :] <= jnp.maximum(query_pos, 0)[:, None])[None]
    vals = all_kv[:, 2 * key_width :].reshape(total, head_count, value_dim)
    maps = [
        weigh(
            query.reshape(rows, head_count, head_dim),
            all_kv[:, m * key_width : (m + 1) * key_width].reshape(total, head_count, head_dim),
            vals,
            visible,
            scale,
        )
        for m, query in enumerate((query_a, query_b))
    ]
    diff_heads = maps[0] - lambdas[None, :, None] * maps[1]
    head_out = rms_scale(diff_heads, head_gain).astype(jnp.bfloat16)
    head_out = head_out.reshape(rows, head_count * value_dim)
    heads = lax.all_gather(head_out, "tp", axis=1, tiled=True)
    attended = jnp.dot(heads, out_rows, preferred_element_type=jnp.float32)
    stream = residual.astype(jnp.float32) + attended
    ffn_in = rms_scale(stream, mix_gain).astype(jnp.bfloat16)

    def convolve(weight, taps):
        projected = jnp.dot(ffn_in, weight, preferred_element_type=jnp.float32)
        projected = jnp.where(query_pos[:, None] >= 0, projected.astype(jnp.bfloat16), 0.0)
        projected = projected.astype(jnp.float32)
        lead = halo - (tap_count - 1)
        result = taps[0][None] * projected[lead : lead + tok_rows]
        for offset in range(1, tap_count):
            start = lead + offset
            result = result + taps[offset][None] * projected[start : start + tok_rows]
        return result

    hidden = jax.nn.silu(convolve(gates, gate_taps)) * convolve(ups, up_taps)
    down = jnp.dot(hidden.astype(jnp.bfloat16), down_weight, preferred_element_type=jnp.float32)
    summed = lax.psum_scatter(
        down.astype(jnp.bfloat16), "tp", scatter_dimension=0, tiled=True
    ).astype(jnp.float32)
    part_rows = tok_rows // tp_count
    own = lax.dynamic_slice_in_dim(stream, halo + tp_rank * part_rows, part_rows, 0)
    return (own + summed).astype(jnp.bfloat16)


def shards(
    q_first,
    k_first,
    q_second,
    k_second,
    values,
    lambdas,
    head_gain,
    out_weight,
    residual_in,
    mix_gain,
    gate_weight,
    up_weight,
    gate_taps,
    up_taps,
    down_weight,
):
    sp_count, tp_count = lax.axis_size("sp"), lax.axis_size("tp")
    tok_rows = q_first.shape[0]
    head_count = lambdas.shape[0]
    tap_count = gate_taps.shape[0]
    halo = halo_of(tok_rows, tap_count)
    layers, sides = layers_of(sp_count, tp_count)

    def across(value, up, flip, wrap=True, keep=lambda l, s: True):
        pairs = []
        for source in range(sp_count):
            l, s = source // sides, source % sides
            target = (l + up) % layers * sides + (s ^ flip)
            if keep(l, s) and (wrap or 0 <= l + up < layers):
                pairs.append((source, target))
        return lax.ppermute(value, "sp", pairs)

    own_kv, tail = pack(k_first, k_second, values, q_first, q_second, residual_in, halo)
    *cuts, taps = cut(gate_weight, up_weight, gate_taps, up_taps, layers, sides)
    shifted = [own_kv]
    shifted += [across(own_kv, k, 0, wrap=False) for k in range(1, layers)]
    blocks = []
    for k, block in enumerate(shifted):
        useful = (lambda l, s: s == 0) if k == 0 else (lambda l, s, k=k: l >= k)
        blocks += [block, across(block, 0, 1, keep=useful)]
    before = lax.ppermute(tail, "sp", [(i, i + 1) for i in range(sp_count - 1)])
    columns = [cuts[0]] + [across(cuts[k], k, 0) for k in range(1, layers)]
    heads = attend(
        lambdas,
        before,
        q_first,
        q_second,
        blocks,
        head_gain,
        head_count,
        values.shape[1],
        sides,
    )
    out_rows = {0: out_weight}
    bit = tp_count // 2
    while bit:
        for slot, block in list(out_rows.items()):
            block = after(block, heads) if slot else block
            out_rows[slot | bit] = swapped(block, "tp", bit)
        bit //= 2
    out_rows = [out_rows[slot] for slot in range(tp_count)]
    own_stream, first_piece, other_pieces = project(
        xor_gather(heads, "tp"),
        out_rows,
        before,
        residual_in,
        mix_gain,
    )
    weights = []
    for k in range(layers):
        block = columns[k]
        if k > 1:
            block = after(block, first_piece)
        weights += [columns[k], across(block, 0, 1)]

    arrived = [None] + [across(first_piece, k, 0) for k in range(1, layers)]
    half = tp_count // 2
    spread = {k: {0: arrived[k]} for k in range(1, layers)}
    for slots in spread.values():
        slots[half] = swapped(slots[0], "tp", half)

    def finished(k, hold):
        slots = spread[k]
        bit = half // 2
        while bit:
            for slot, block in list(slots.items()):
                block = block if hold is None else after(block, hold)
                slots[slot | bit] = swapped(block, "tp", bit)
            bit //= 2
        return [slots[slot] for slot in range(tp_count)]

    far = layers - 1
    early = {0: [first_piece, other_pieces], far: finished(far, None)}
    hiddens = {}
    for k, pieces in early.items():
        (hiddens[k],) = mixer({k: pieces}, weights, taps, tp_count, layers, tok_rows)
    for k in range(far - 1, 0, -1):
        late = {k: finished(k, None)}
        hiddens.update(zip(late, mixer(late, weights, taps, tp_count, layers, tok_rows)))
    hiddens = [across(hiddens[k], -k, 0) if k else hiddens[k] for k in range(layers)]
    mixed, *parts = project_down(hiddens, down_weight, own_stream, tp_count, sides)
    for bit in reversed(range(1, tp_count)):
        part = swapped(parts[bit - 1], "tp", bit)
        mixed = mixed + part.astype(jnp.float32)
    return mixed.astype(jnp.bfloat16)


def solution(mesh):
    in_specs = (
        P("sp", "tp"),
        P("sp", "tp"),
        P("sp", "tp"),
        P("sp", "tp"),
        P("sp", "tp"),
        P("tp"),
        P(),
        P("tp", None),
        P("sp", None),
        P(),
        P("sp", "tp"),
        P("sp", "tp"),
        P(None, "tp"),
        P(None, "tp"),
        P("tp", None),
    )
    out_specs = P(("sp", "tp"), None)
    sizes = mesh.shape
    grid = layers_of(sizes["sp"], sizes["tp"])
    if not grid:
        return jax.shard_map(
            local_shards, mesh=mesh, in_specs=in_specs, out_specs=out_specs, check_vma=False
        )

    return jax.shard_map(shards, mesh=mesh, in_specs=in_specs, out_specs=out_specs, check_vma=False)
```

```python
import functools

import jax
import jax.numpy as jnp
from jax import lax
from jax.experimental import pallas as pl
from jax.experimental.pallas import tpu as pltpu
from jax.sharding import PartitionSpec as P


norm_eps = 1e-06
far_below = -1e30
HALO_TILE = 8


def swapped(value, axis, bit):
    count = lax.axis_size(axis)
    return lax.ppermute(value, axis, [(i, i ^ bit) for i in range(count)])


def xor_gather(value, axis):
    count = lax.axis_size(axis)
    slots = {0: value}
    bits = [1 << b for b in range((count - 1).bit_length())]
    for bit in reversed(bits):
        for slot, block in list(slots.items()):
            slots[slot | bit] = swapped(block, axis, bit)
    return [slots[i] for i in range(count)]


def after(value, *others):
    return lax.optimization_barrier((value,) + others)[0]


def rms_scale(field, gain):
    return field * lax.rsqrt(jnp.mean(field * field, axis=-1, keepdims=True) + norm_eps) * gain


def whole(count):
    return [pl.BlockSpec(memory_space=pltpu.VMEM)] * count


def params_for(mebibytes):
    return pltpu.CompilerParams(vmem_limit_bytes=mebibytes * 2**20)


def attend_kernel(head_count, block_count, sides, scale, *refs):
    lambda_ref, before_ref, qa_ref, qb_ref = refs[:4]
    kv_refs = refs[4 : 4 + block_count]
    gain_ref, out_ref, key_ref, query_ref, bias_ref, score_ref, sems = refs[4 + block_count :]
    place = lax.axis_index("sp")
    layer, side = place // sides, lax.rem(place, sides)
    tok_rows, key_width = qa_ref.shape
    rows = out_ref.shape[0]
    halo = rows - tok_rows
    head_dim = key_width // head_count
    value_dim = out_ref.shape[1] // head_count
    copies = [
        pltpu.make_async_copy(
            ref, query_ref.at[pl.ds(halo, tok_rows), m * key_width : (m + 1) * key_width], sems.at[m]
        )
        for m, ref in enumerate((qa_ref, qb_ref))
    ]
    for copy in copies:
        copy.start()
    shape = (rows, tok_rows)
    ahead = lax.broadcasted_iota(jnp.int32, shape, 0) - halo
    spread = jnp.maximum(ahead + place * tok_rows, 0) - lax.broadcasted_iota(jnp.int32, shape, 1)
    for b, kv_ref in enumerate(kv_refs):
        span = slice(b * tok_rows, (b + 1) * tok_rows)
        key_ref[span, :] = kv_ref[...]
        source = (layer - b // sides) * sides + (side ^ (b % sides))
        limit = jnp.where(source >= 0, source * tok_rows, 2**30)
        bias_ref[:, span] = jnp.where(spread >= limit, 0.0, far_below)
    query_ref[:halo, :] = before_ref[:, : 2 * key_width]
    for copy in copies:
        copy.wait()
    for h in range(head_count):
        totals = []
        for m in range(2):
            start = m * key_width + h * head_dim
            scores = lax.dot_general(
                query_ref[:, start : start + head_dim],
                key_ref[:, start : start + head_dim],
                (((1,), (1,)), ((), ())),
                preferred_element_type=jnp.float32,
            )
            scores = scores * scale + bias_ref[...]
            weights = jnp.exp(scores - jnp.max(scores, axis=-1, keepdims=True))
            totals.append(jnp.sum(weights, axis=-1, keepdims=True))
            score_ref[h, m * rows : (m + 1) * rows, :] = weights.astype(jnp.bfloat16)
        first = 2 * key_width + h * value_dim
        accum = jnp.dot(
            score_ref[h], key_ref[:, first : first + value_dim], preferred_element_type=jnp.float32
        )
        field = accum[:rows] / totals[0] - lambda_ref[h] * (accum[rows:] / totals[1])
        norm = lax.rsqrt(jnp.mean(field * field, axis=-1, keepdims=True) + norm_eps)
        out_ref[:, h * value_dim : (h + 1) * value_dim] = (field * norm * gain_ref[...]).astype(
            out_ref.dtype
        )


def attend(lambdas, before, q_first, q_second, blocks, head_gain, head_count, width, sides):
    tok_rows, key_width = q_first.shape
    rows = tok_rows + before.shape[0]
    count = len(blocks)
    scale = (key_width // head_count) ** (-0.5)
    keys = count * tok_rows
    smem = pl.BlockSpec(memory_space=pltpu.SMEM)
    return pl.pallas_call(
        functools.partial(attend_kernel, head_count, count, sides, scale),
        out_shape=jax.ShapeDtypeStruct((rows, width), jnp.bfloat16),
        in_specs=[smem]
        + whole(1)
        + [pl.BlockSpec(memory_space=pl.ANY)] * 2
        + whole(count + 1),
        out_specs=pl.BlockSpec(memory_space=pltpu.VMEM),
        scratch_shapes=[
            pltpu.VMEM((keys, blocks[0].shape[1]), jnp.bfloat16),
            pltpu.VMEM((rows, 2 * key_width), jnp.bfloat16),
            pltpu.VMEM((rows, keys), jnp.float32),
            pltpu.VMEM((head_count, 2 * rows, keys), jnp.bfloat16),
            pltpu.SemaphoreType.DMA((2,)),
        ],
        compiler_params=params_for(60),
        cost_estimate=pl.CostEstimate(
            flops=4 * rows * keys * (key_width + width),
            bytes_accessed=2 * keys * blocks[0].shape[1],
            transcendentals=2 * head_count * rows * keys,
        ),
        name="attend",
    )(lambdas, before, q_first, q_second, *blocks, head_gain[None])


def project_kernel(slots, part_rows, *refs):
    head_refs, weight_refs = refs[:slots], refs[slots : 2 * slots]
    before_ref, residual_ref, gain_ref, part_ref, first_ref, rest_ref = refs[2 * slots :][:6]
    stream_ref, held_ref, rows_ref, sems = refs[2 * slots + 6 :]
    copies = [
        pltpu.make_async_copy(weight_refs[slot], rows_ref.at[slot], sems.at[slot])
        for slot in range(slots)
    ]
    copy = pltpu.make_async_copy(residual_ref, held_ref, sems.at[slots])
    for started in copies:
        started.start()
    copy.start()
    halo, skip = before_ref.shape
    skip = skip - stream_ref.shape[1]
    total = None
    for slot in range(slots):
        copies[slot].wait()
        product = jnp.dot(
            head_refs[slot][...], rows_ref[slot], preferred_element_type=jnp.float32
        )
        total = product if total is None else total + product
    stream_ref[:halo] = total[:halo] + before_ref[:, skip:].astype(jnp.float32)
    copy.wait()
    stream_ref[halo:] = total[halo:] + held_ref[...].astype(jnp.float32)
    rank = lax.axis_index("tp")
    part_ref[...] = stream_ref[pl.ds(pl.multiple_of(halo + rank * part_rows, 8), part_rows), :]
    stream = stream_ref[...]
    norm = lax.rsqrt(jnp.mean(stream * stream, axis=-1, keepdims=True) + norm_eps)
    quarter = first_ref.shape[1]
    for slot in range(slots):
        columns = pl.ds(pl.multiple_of((rank ^ slot) * quarter, 128), quarter)
        piece = (stream_ref[:, columns] * norm * gain_ref[:, columns]).astype(jnp.bfloat16)
        if slot == 0:
            first_ref[...] = piece
        else:
            rest_ref[slot - 1] = piece


def project(heads, weights, before, residual, gain):
    slots = len(heads)
    rows = heads[0].shape[0]
    tok_rows, columns = residual.shape
    part = tok_rows // slots
    quarter = columns // slots
    vmem = pl.BlockSpec(memory_space=pltpu.VMEM)
    return pl.pallas_call(
        functools.partial(project_kernel, slots, part),
        out_shape=(
            jax.ShapeDtypeStruct((part, columns), jnp.float32),
            jax.ShapeDtypeStruct((rows, quarter), jnp.bfloat16),
            jax.ShapeDtypeStruct((slots - 1, rows, quarter), jnp.bfloat16),
        ),
        in_specs=whole(slots)
        + [pl.BlockSpec(memory_space=pl.ANY)] * slots
        + whole(1)
        + [pl.BlockSpec(memory_space=pl.ANY), vmem],
        out_specs=(vmem,) * 3,
        scratch_shapes=[
            pltpu.VMEM((rows, columns), jnp.float32),
            pltpu.VMEM(residual.shape, residual.dtype),
            pltpu.VMEM((slots,) + weights[0].shape, weights[0].dtype),
            pltpu.SemaphoreType.DMA((slots + 1,)),
        ],
        compiler_params=params_for(60),
        cost_estimate=pl.CostEstimate(
            flops=2 * rows * columns * slots * heads[0].shape[1],
            bytes_accessed=2 * columns * slots * heads[0].shape[1],
            transcendentals=rows,
        ),
        name="project",
    )(*heads, *weights, before, residual, gain[None])


def copy_all(pairs, sems):
    copies = [
        pltpu.make_async_copy(source, target, sems.at[i]) for i, (source, target) in enumerate(pairs)
    ]
    for copy in copies:
        copy.start()
    for copy in copies:
        copy.wait()


def pack_kernel(k_first_ref, k_second_ref, values_ref, qa_ref, qb_ref, rest_ref, kv_ref, tail_ref, sems):
    rows, width = k_first_ref.shape
    halo = tail_ref.shape[0]
    last = pl.ds(rows - halo, halo)
    copy_all(
        [
            (k_first_ref, kv_ref.at[:, :width]),
            (k_second_ref, kv_ref.at[:, width : 2 * width]),
            (values_ref, kv_ref.at[:, 2 * width :]),
            (qa_ref.at[last, :], tail_ref.at[:, :width]),
            (qb_ref.at[last, :], tail_ref.at[:, width : 2 * width]),
            (rest_ref.at[last, :], tail_ref.at[:, 2 * width :]),
        ],
        sems,
    )


def pack(k_first, k_second, values, q_first, q_second, residual, halo):
    tok_rows, width = k_first.shape
    return pl.pallas_call(
        pack_kernel,
        out_shape=(
            jax.ShapeDtypeStruct((tok_rows, 2 * width + values.shape[1]), k_first.dtype),
            jax.ShapeDtypeStruct((halo, 2 * width + residual.shape[1]), residual.dtype),
        ),
        in_specs=[pl.BlockSpec(memory_space=pl.ANY)] * 6,
        out_specs=tuple(whole(2)),
        scratch_shapes=[pltpu.SemaphoreType.DMA((6,))],
        compiler_params=params_for(60),
        name="pack",
    )(k_first, k_second, values, q_first, q_second, residual)


def cut_kernel(layers, sides, gate_ref, up_ref, gate_taps_ref, up_taps_ref, *refs):
    out_refs, (taps_ref, gate_held, up_held, sems) = refs[:layers], refs[layers:]
    share = gate_ref.shape[1] // layers
    copy_all([(gate_ref, gate_held), (up_ref, up_held)], sems)
    layer = lax.axis_index("sp") // sides
    for own in range(layers):

        @pl.when(layer == own)
        def _():
            for k, out_ref in enumerate(out_refs):
                start = (own + k) % layers * share
                out_ref[:, :share] = gate_held[:, start : start + share]
                out_ref[:, share:] = up_held[:, start : start + share]
            start = own * share
            taps_ref[:, :share] = gate_taps_ref[:, start : start + share]
            taps_ref[:, share:] = up_taps_ref[:, start : start + share]


def cut(gate_weight, up_weight, gate_taps, up_taps, layers, sides):
    depth, width = gate_weight.shape
    share = 2 * (width // layers)
    return pl.pallas_call(
        functools.partial(cut_kernel, layers, sides),
        out_shape=[jax.ShapeDtypeStruct((depth, share), gate_weight.dtype)] * layers
        + [jax.ShapeDtypeStruct((gate_taps.shape[0], share), gate_taps.dtype)],
        in_specs=[pl.BlockSpec(memory_space=pl.ANY)] * 2 + whole(2),
        out_specs=whole(layers + 1),
        scratch_shapes=[
            pltpu.VMEM(gate_weight.shape, gate_weight.dtype),
            pltpu.VMEM(up_weight.shape, up_weight.dtype),
            pltpu.SemaphoreType.DMA((2,)),
        ],
        compiler_params=params_for(60),
        cost_estimate=pl.CostEstimate(
            flops=4 * depth * width, bytes_accessed=8 * depth * width, transcendentals=0
        ),
        name="cut",
    )(gate_weight, up_weight, gate_taps, up_taps)


def mixer_kernel(slots, layers, sides, tok_rows, aboves, counts, *refs):
    count = layers * sides
    taken = sum(counts)
    piece_refs, weight_refs = refs[:taken], refs[taken : taken + count]
    taps_ref, *out_refs = refs[taken + count : -2]
    act_ref, pre_ref = refs[-2:]
    tap_count = taps_ref.shape[0]
    rows = pre_ref.shape[0]
    share = out_refs[0].shape[1]
    halo = rows - tok_rows
    place, rank = lax.axis_index("sp"), lax.axis_index("tp")
    layer, side = place // sides, lax.rem(place, sides)
    depth = weight_refs[0].shape[0]
    per_slot = count // slots
    begin = 0
    for above, number, out_ref in zip(aboves, counts, out_refs):
        pieces = []
        for ref in piece_refs[begin : begin + number]:
            pieces += [ref] if len(ref.shape) == 2 else [ref.at[i] for i in range(ref.shape[0])]
        begin += number
        for slot, piece in enumerate(pieces):
            for i in range(per_slot):
                act_ref[slot * per_slot + i] = piece[:, i * depth : (i + 1) * depth]
        total = None
        for j, weight_ref in enumerate(weight_refs):
            block = lax.rem(layer + layers - j // sides, layers) * sides + (side ^ (j % sides))
            slot = (block // per_slot) ^ rank
            act = act_ref[slot * per_slot + lax.rem(block, per_slot)]
            product = jnp.dot(act, weight_ref[...], preferred_element_type=jnp.float32)
            total = product if total is None else total + product
        source = lax.rem(layer + layers - above, layers) * sides + side
        position = lax.broadcasted_iota(jnp.int32, (rows, 1), 0) - halo + source * tok_rows
        total = jnp.where(position >= 0, total, 0.0)
        pre_ref[...] = total.astype(jnp.bfloat16).astype(jnp.float32)
        lead = halo - (tap_count - 1)
        convolved = None
        for k in range(tap_count):
            term = taps_ref[k : k + 1, :] * pre_ref[lead + k : lead + k + tok_rows, :]
            convolved = term if convolved is None else convolved + term
        gate = convolved[:, :share]
        out_ref[...] = (gate / (1.0 + jnp.exp(-gate)) * convolved[:, share:]).astype(out_ref.dtype)


def mixer(blocks, weights, taps, slots, layers, tok_rows):
    aboves = tuple(blocks)
    counts = tuple(len(pieces) for pieces in blocks.values())
    arrays = [piece for pieces in blocks.values() for piece in pieces]
    rows = arrays[0].shape[-2]
    depth, columns = weights[0].shape
    count = len(weights)
    return pl.pallas_call(
        functools.partial(
            mixer_kernel, slots, layers, count // layers, tok_rows, aboves, counts
        ),
        out_shape=[jax.ShapeDtypeStruct((tok_rows, columns // 2), jnp.bfloat16)] * len(aboves),
        in_specs=whole(len(arrays) + count + 1),
        out_specs=whole(len(aboves)),
        scratch_shapes=[
            pltpu.VMEM((count, rows, depth), jnp.bfloat16),
            pltpu.VMEM((rows, columns), jnp.float32),
        ],
        compiler_params=params_for(24),
        cost_estimate=pl.CostEstimate(
            flops=2 * len(aboves) * rows * columns * count * depth,
            bytes_accessed=2 * columns * count * depth,
            transcendentals=len(aboves) * rows * columns // 2,
        ),
        name="mixer",
    )(*arrays, *weights, taps)


def down_kernel(layers, sides, *refs):
    hidden_refs, (weight_ref, stream_ref), out_refs = refs[:layers], refs[layers : layers + 2], refs[layers + 2 :]
    own_ref, *part_refs = out_refs[:-1]
    total_ref = out_refs[-1]
    share = hidden_refs[0].shape[1]
    layer, rank = lax.axis_index("sp") // sides, lax.axis_index("tp")
    total = None
    for k, hidden_ref in enumerate(hidden_refs):
        start = pl.multiple_of(lax.rem(layer + k, layers) * share, 16)
        product = jnp.dot(
            hidden_ref[...], weight_ref[pl.ds(start, share), :], preferred_element_type=jnp.float32
        )
        total = product if total is None else total + product
    total_ref[...] = total
    rows = own_ref.shape[0]
    own_ref[...] = stream_ref[...] + total_ref[pl.ds(pl.multiple_of(rank * rows, 8), rows), :]
    odd_ref, even_ref = part_refs if len(part_refs) == 2 else (part_refs[0], None)
    for slot in range(1, total_ref.shape[0] // rows):
        start = pl.multiple_of((rank ^ slot) * rows, 8)
        target = odd_ref.at[slot // 2] if slot % 2 else even_ref.at[slot // 2 - 1]
        target[...] = total_ref[pl.ds(start, rows), :].astype(target.dtype)


def project_down(hiddens, weight, stream, slots, sides):
    rows, columns = stream.shape
    layers = len(hiddens)
    return pl.pallas_call(
        functools.partial(down_kernel, layers, sides),
        out_shape=[jax.ShapeDtypeStruct(stream.shape, jnp.float32)]
        + [jax.ShapeDtypeStruct((slots // 2, rows, columns), jnp.bfloat16)]
        + [jax.ShapeDtypeStruct((slots // 2 - 1, rows, columns), jnp.float32)] * (slots > 2),
        in_specs=whole(layers + 2),
        out_specs=whole(2 + (slots > 2)),
        scratch_shapes=[
            pltpu.VMEM((rows * slots, columns), jnp.float32),
        ],
        compiler_params=params_for(18),
        cost_estimate=pl.CostEstimate(
            flops=2 * rows * slots * weight.size,
            bytes_accessed=2 * weight.size,
            transcendentals=0,
        ),
        name="down",
    )(*hiddens, weight, stream)


def layers_of(sp_count, tp_count):
    if sp_count > 8 or sp_count % 2 or tp_count & (tp_count - 1):
        return None
    layers = sp_count // 2
    if layers < 2 or (2 * layers) % tp_count:
        return None
    return layers, 2


def halo_of(tok_rows, tap_count):
    return min(tok_rows, -(-(tap_count - 1) // HALO_TILE) * HALO_TILE)


def weigh(queries, keys, vals, visible, scale):
    scores = jnp.einsum("qhd,khd->hqk", queries, keys, preferred_element_type=jnp.float32) * scale
    masked = jnp.where(visible, scores, far_below)
    peaks = jnp.max(masked, axis=-1, keepdims=True)
    weights = jnp.where(visible, jnp.exp(masked - peaks), 0.0)
    totals = jnp.sum(weights, axis=-1)
    accum = jnp.einsum(
        "hqk,khv->qhv", weights.astype(jnp.bfloat16), vals, preferred_element_type=jnp.float32
    )
    return accum / totals.T[..., None]


def local_shards(
    q_first,
    k_first,
    q_second,
    k_second,
    values,
    lambdas,
    head_gain,
    out_weight,
    residual_in,
    mix_gain,
    gate_weight,
    up_weight,
    gate_taps,
    up_taps,
    down_weight,
):
    sp_count, tp_count = lax.axis_size("sp"), lax.axis_size("tp")
    sp_rank, tp_rank = lax.axis_index("sp"), lax.axis_index("tp")
    tok_rows = q_first.shape[0]
    head_count = lambdas.shape[0]
    key_width = q_first.shape[1]
    head_dim = key_width // head_count
    value_dim = values.shape[1] // head_count
    tap_count, _ = gate_taps.shape
    halo = halo_of(tok_rows, tap_count)
    rows = tok_rows + halo
    scale = head_dim ** (-0.5)
    own_kv = jnp.concatenate((k_first, k_second, values), axis=1)
    all_kv = lax.all_gather(own_kv, "sp", axis=0, tiled=True)
    tail = jnp.concatenate((q_first, q_second, residual_in), axis=1)[tok_rows - halo :]
    before = lax.ppermute(tail, "sp", [(i, i + 1) for i in range(sp_count - 1)])
    out_rows = lax.all_gather(out_weight, "tp", axis=0, tiled=True)
    gates = lax.all_gather(gate_weight, "sp", axis=0, tiled=True)
    ups = lax.all_gather(up_weight, "sp", axis=0, tiled=True)
    query_pos = sp_rank * tok_rows - halo + jnp.arange(rows, dtype=jnp.int32)
    query_a = jnp.concatenate((before[:, :key_width], q_first), axis=0)
    query_b = jnp.concatenate((before[:, key_width : 2 * key_width], q_second), axis=0)
    residual = jnp.concatenate((before[:, 2 * key_width :], residual_in), axis=0)
    total = all_kv.shape[0]
    key_pos = jnp.arange(total, dtype=jnp.int32)
    visible = (key_pos[None, :] <= jnp.maximum(query_pos, 0)[:, None])[None]
    vals = all_kv[:, 2 * key_width :].reshape(total, head_count, value_dim)
    maps = [
        weigh(
            query.reshape(rows, head_count, head_dim),
            all_kv[:, m * key_width : (m + 1) * key_width].reshape(total, head_count, head_dim),
            vals,
            visible,
            scale,
        )
        for m, query in enumerate((query_a, query_b))
    ]
    diff_heads = maps[0] - lambdas[None, :, None] * maps[1]
    head_out = rms_scale(diff_heads, head_gain).astype(jnp.bfloat16)
    head_out = head_out.reshape(rows, head_count * value_dim)
    heads = lax.all_gather(head_out, "tp", axis=1, tiled=True)
    attended = jnp.dot(heads, out_rows, preferred_element_type=jnp.float32)
    stream = residual.astype(jnp.float32) + attended
    ffn_in = rms_scale(stream, mix_gain).astype(jnp.bfloat16)

    def convolve(weight, taps):
        projected = jnp.dot(ffn_in, weight, preferred_element_type=jnp.float32)
        projected = jnp.where(query_pos[:, None] >= 0, projected.astype(jnp.bfloat16), 0.0)
        projected = projected.astype(jnp.float32)
        lead = halo - (tap_count - 1)
        result = taps[0][None] * projected[lead : lead + tok_rows]
        for offset in range(1, tap_count):
            start = lead + offset
            result = result + taps[offset][None] * projected[start : start + tok_rows]
        return result

    hidden = jax.nn.silu(convolve(gates, gate_taps)) * convolve(ups, up_taps)
    down = jnp.dot(hidden.astype(jnp.bfloat16), down_weight, preferred_element_type=jnp.float32)
    summed = lax.psum_scatter(
        down.astype(jnp.bfloat16), "tp", scatter_dimension=0, tiled=True
    ).astype(jnp.float32)
    part_rows = tok_rows // tp_count
    own = lax.dynamic_slice_in_dim(stream, halo + tp_rank * part_rows, part_rows, 0)
    return (own + summed).astype(jnp.bfloat16)


def shards(
    q_first,
    k_first,
    q_second,
    k_second,
    values,
    lambdas,
    head_gain,
    out_weight,
    residual_in,
    mix_gain,
    gate_weight,
    up_weight,
    gate_taps,
    up_taps,
    down_weight,
):
    sp_count, tp_count = lax.axis_size("sp"), lax.axis_size("tp")
    tok_rows = q_first.shape[0]
    head_count = lambdas.shape[0]
    tap_count = gate_taps.shape[0]
    halo = halo_of(tok_rows, tap_count)
    layers, sides = layers_of(sp_count, tp_count)

    def across(value, up, flip, wrap=True, keep=lambda l, s: True):
        pairs = []
        for source in range(sp_count):
            l, s = source // sides, source % sides
            target = (l + up) % layers * sides + (s ^ flip)
            if keep(l, s) and (wrap or 0 <= l + up < layers):
                pairs.append((source, target))
        return lax.ppermute(value, "sp", pairs)

    own_kv, tail = pack(k_first, k_second, values, q_first, q_second, residual_in, halo)
    *cuts, taps = cut(gate_weight, up_weight, gate_taps, up_taps, layers, sides)
    shifted = [own_kv]
    shifted += [across(own_kv, k, 0, wrap=False) for k in range(1, layers)]
    blocks = []
    for k, block in enumerate(shifted):
        useful = (lambda l, s: s == 0) if k == 0 else (lambda l, s, k=k: l >= k)
        blocks += [block, across(block, 0, 1, keep=useful)]
    before = lax.ppermute(tail, "sp", [(i, i + 1) for i in range(sp_count - 1)])
    columns = [cuts[0]] + [across(cuts[k], k, 0) for k in range(1, layers)]
    heads = attend(
        lambdas,
        before,
        q_first,
        q_second,
        blocks,
        head_gain,
        head_count,
        values.shape[1],
        sides,
    )
    out_rows = {0: out_weight}
    bit = tp_count // 2
    while bit:
        for slot, block in list(out_rows.items()):
            block = after(block, heads) if slot else block
            out_rows[slot | bit] = swapped(block, "tp", bit)
        bit //= 2
    out_rows = [out_rows[slot] for slot in range(tp_count)]
    own_stream, first_piece, other_pieces = project(
        xor_gather(heads, "tp"),
        out_rows,
        before,
        residual_in,
        mix_gain,
    )
    weights = []
    for k in range(layers):
        block = columns[k]
        if k > 1:
            block = after(block, first_piece)
        weights += [columns[k], across(block, 0, 1)]

    arrived = [None] + [across(first_piece, k, 0) for k in range(1, layers)]
    half = tp_count // 2
    spread = {k: {0: arrived[k]} for k in range(1, layers)}
    for slots in spread.values():
        slots[half] = swapped(slots[0], "tp", half)

    def finished(k, hold):
        slots = spread[k]
        bit = half // 2
        while bit:
            for slot, block in list(slots.items()):
                block = block if hold is None else after(block, hold)
                slots[slot | bit] = swapped(block, "tp", bit)
            bit //= 2
        return [slots[slot] for slot in range(tp_count)]

    far = layers - 1
    early = {0: [first_piece, other_pieces], far: finished(far, None)}
    hiddens = {}
    for k, pieces in early.items():
        (hiddens[k],) = mixer({k: pieces}, weights, taps, tp_count, layers, tok_rows)
    for k in range(far - 1, 0, -1):
        late = {k: finished(k, None)}
        hiddens.update(zip(late, mixer(late, weights, taps, tp_count, layers, tok_rows)))
    hiddens = [across(hiddens[k], -k, 0) if k else hiddens[k] for k in range(layers)]
    mixed, odd, *even = project_down(hiddens, down_weight, own_stream, tp_count, sides)
    got = swapped(odd, "tp", 1).astype(jnp.float32)
    mixed = mixed + got[0]
    held = even[0] + got[1:] if even else None
    bit = 2
    while bit < tp_count:
        got = swapped(held[::2].astype(jnp.bfloat16), "tp", bit).astype(jnp.float32)
        mixed = mixed + got[0]
        held = held[1::2] + got[1:]
        bit *= 2
    return mixed.astype(jnp.bfloat16)


def solution(mesh):
    in_specs = (
        P("sp", "tp"),
        P("sp", "tp"),
        P("sp", "tp"),
        P("sp", "tp"),
        P("sp", "tp"),
        P("tp"),
        P(),
        P("tp", None),
        P("sp", None),
        P(),
        P("sp", "tp"),
        P("sp", "tp"),
        P(None, "tp"),
        P(None, "tp"),
        P("tp", None),
    )
    out_specs = P(("sp", "tp"), None)
    sizes = mesh.shape
    grid = layers_of(sizes["sp"], sizes["tp"])
    if not grid:
        return jax.shard_map(
            local_shards, mesh=mesh, in_specs=in_specs, out_specs=out_specs, check_vma=False
        )

    return jax.shard_map(shards, mesh=mesh, in_specs=in_specs, out_specs=out_specs, check_vma=False)
```
